32 devices in a mesh: sp: 8 (over z, x), tp: 4 (over y, core).
Axes of the slice: x: 2, y: 2, z: 4, core: 2. Of those that a mesh axis runs over, the one named last changes fastest.
Arguments:
- tokens: bfloat16 [8, 768, 2048], P('sp', 'tp'), may hold values from -100 to 100
- norm_gain: float32 [2048], replicated, may hold values from 0.1 to 1.9
- key_weight: bfloat16 [2048, 1024], P('sp', 'tp'), may hold values from -0.125 to 0.125
- value_weight: bfloat16 [2048, 1024], P('sp', 'tp'), may hold values from -0.125 to 0.125
- cum_gate: float32 [8, 32, 768], P('sp', None, 'tp'), may hold values from -119 to 0, as said below
- new_gate: float32 [8, 32], P('sp', 'tp'), may hold values from -119 to 0
- new_query: bfloat16 [8, 2048], P('sp', 'tp'), may hold values from -128 to 128
- new_kv: bfloat16 [8, 16, 128], P('sp', 'tp'), may hold values from -4 to 4
Outputs:
- kv_cache: bfloat16 [8, 16, 768, 128], P('sp', 'tp')
- gate_log_cache: float32 [8, 32, 768], P('sp', 'tp')
- read_out: bfloat16 [8, 2048], P('sp', 'tp')
The draws below stay inside these ranges and needn't reach their ends.
Inputs may be any that keep to these rules, and one draw needn't show every extreme that they name: Along positions cum_gate never rises; new_gate is at most the last position's value of its prompt and head.
All inputs are finite; a program needn't handle non-finite values.
Results may differ from the reference program's by a relative error of at most 0.0071.
Values may be sent and summed in bfloat16 or wider, within the bound.
A program may use at most 64 MiB of HBM per device.

```python
import math
import jax
import jax.numpy as jnp
from jax import lax

D = 2048
HEADS = 32
KV_HEADS = 16
HEAD = 64
POS_DEV = 192
SEQS = 8
PROMPT_LENGTH = 768


def gate_table(key):
    key_slow = jax.random.fold_in(key, 101)
    key_rate = jax.random.fold_in(key, 102)
    key_block = jax.random.fold_in(key, 103)
    key_place = jax.random.fold_in(key, 104)
    key_random_split = jax.random.fold_in(key, 105)
    key_layer_count = jax.random.fold_in(key, 106)
    slow_share = 0.5
    slow = jax.random.uniform(key_slow, (SEQS, HEADS, 1), jnp.float32) < slow_share
    scatter_update = jnp.exp(jax.random.uniform(key_rate, (SEQS, HEADS, 1), jnp.float32, jnp.log(0.5), jnp.log(2.0)))
    base = jnp.where(slow, scatter_update / PROMPT_LENGTH, scatter_update * 0.8 / 40.0)
    blocks = PROMPT_LENGTH // POS_DEV + 1
    block_table = jnp.exp(jax.random.uniform(key_block, (SEQS, 1, blocks), jnp.float32, jnp.log(0.5), jnp.log(2.0)))
    block_rate = jnp.repeat(block_table, POS_DEV, axis=2)[:, :, :PROMPT_LENGTH + 1]
    place = jax.random.uniform(key_place, (SEQS, HEADS, PROMPT_LENGTH + 1), jnp.float32, 0.3, 1.7)
    logs = -base * block_rate * place
    slot_locations = jax.random.randint(key_random_split, (4,), 0, PROMPT_LENGTH)
    hit = jnp.any(jnp.arange(PROMPT_LENGTH + 1)[:, None] == slot_locations[None, :], axis=1)
    depth = jnp.log(jax.random.uniform(key_layer_count, (SEQS, HEADS, 1), jnp.float32, 0.5, 0.8))
    logs = logs + jnp.where(hit[None, None, :] & slow, depth, 0.0)
    return jnp.cumsum(logs, axis=2)


def draw_cum_gate(key, part):
    return gate_table(key)[:, :, :PROMPT_LENGTH]


def draw_new_gate(key, part):
    return gate_table(key)[:, :, PROMPT_LENGTH]


def draw_tokens(key, part):
    key_main = jax.random.fold_in(key, 201)
    column_scale = 0.5 * 4.0 ** (jnp.arange(D, dtype=jnp.float32) / D)
    values = jax.random.truncated_normal(key_main, -4.0, 4.0, (SEQS, PROMPT_LENGTH, D), jnp.float32) * column_scale
    return values.astype(jnp.bfloat16)


def updated_page_table(key):
    key_kv = jax.random.fold_in(key, 301)
    key_query = jax.random.fold_in(key, 302)
    fresh_kv = jax.random.truncated_normal(key_kv, -4.0, 4.0, (SEQS, KV_HEADS, 2 * HEAD), jnp.float32)
    query = jax.random.truncated_normal(key_query, -4.0, 4.0, (SEQS, HEADS, HEAD), jnp.float32)
    return (query.reshape(SEQS, HEADS * HEAD), fresh_kv)


def draw_new_query(key, part):
    return updated_page_table(jax.random.fold_in(key, 300))[0].astype(jnp.bfloat16)


def draw_new_kv(key, part):
    return updated_page_table(jax.random.fold_in(key, 300))[1].astype(jnp.bfloat16)


def level_of(key, dims, shards, low, high):
    def one(dim, shards_of):
        steps = jax.random.uniform(jax.random.fold_in(jax.random.fold_in(key, 6), dim), (shards_of,), jnp.float32, low / len(shards), high / len(shards))
        return jnp.repeat(jnp.exp(steps), dims[dim] // shards_of).reshape((-1,) + (1,) * (len(dims) - dim - 1))

    gain = one(*shards[0])
    for cut in shards[1:]:
        gain = gain * one(*cut)
    return gain


def normal_values(key, dims, deviation, bound, split=(), held_as=jnp.bfloat16):
    factor_of = level_of(key, dims, split, -0.22, 0.18) if split else 1.0
    values = jax.random.normal(key, dims, jnp.float32) * deviation * factor_of
    return jnp.minimum(jnp.maximum(values, -bound), bound).astype(held_as)


def setup_inputs(seed: int = 0) -> dict:
    key_of = jax.random.split(jax.random.key(seed), 9)
    return {
        "tokens": draw_tokens(jax.random.fold_in(key_of[8], 71), 0),
        "norm_gain": jnp.clip(1.0 + 0.18 * jax.random.normal(key_of[1], (D,), jnp.float32), 0.1, 1.9),
        "key_weight": normal_values(key_of[2], (D, KV_HEADS * HEAD), D ** -0.5, 0.125, ((0, 8), (1, 4))),
        "value_weight": normal_values(key_of[3], (D, KV_HEADS * HEAD), D ** -0.5, 0.125, ((0, 8), (1, 4))),
        "cum_gate": draw_cum_gate(jax.random.fold_in(key_of[8], 71), 0),
        "new_gate": draw_new_gate(jax.random.fold_in(key_of[8], 71), 0),
        "new_query": draw_new_query(jax.random.fold_in(key_of[8], 71), 0),
        "new_kv": draw_new_kv(jax.random.fold_in(key_of[8], 71), 0),
    }


def reference(tokens, norm_gain, key_weight, value_weight, cum_gate, new_gate, new_query, new_kv):
    scale_factor = 1.0 / math.sqrt(HEAD)
    group = HEADS // KV_HEADS

    def one_prompt(inputs):
        rows, gate_rows, fresh_gate, fresh_query, fresh_kv = inputs
        length = rows.shape[0]
        widened = rows.astype(jnp.float32)
        inv_rms = lax.rsqrt(lax.optimization_barrier(jnp.mean(widened * widened, axis=1, keepdims=True)) + 1e-06)
        scaled = (widened * norm_gain).astype(jnp.bfloat16)
        keys = (jnp.dot(scaled, key_weight, preferred_element_type=jnp.float32) * inv_rms).astype(jnp.bfloat16)
        values = (jnp.dot(scaled, value_weight, preferred_element_type=jnp.float32) * inv_rms).astype(jnp.bfloat16)
        key_heads = keys.reshape(length, KV_HEADS, HEAD)
        value_heads = values.reshape(length, KV_HEADS, HEAD)
        cache = jnp.transpose(jnp.concatenate([key_heads, value_heads], axis=2), (1, 0, 2))
        query = fresh_query.astype(jnp.float32).reshape(KV_HEADS, group, HEAD)
        own_key = fresh_kv[:, :HEAD].astype(jnp.float32)
        own_value = fresh_kv[:, HEAD:].astype(jnp.float32)
        score = jnp.einsum('tkd,kgd->kgt', key_heads.astype(jnp.float32), query) * scale_factor
        score = score + fresh_gate.reshape(KV_HEADS, group)[:, :, None] - gate_rows.reshape(KV_HEADS, group, length)
        own = lax.optimization_barrier(jnp.sum(query * own_key[:, None, :], axis=2)) * scale_factor
        top = jnp.maximum(lax.optimization_barrier(jnp.max(score, axis=2)), own)
        expo = jnp.exp(score - top[:, :, None])
        own_factor = jnp.exp(own - top)
        total = lax.optimization_barrier(jnp.sum(expo, axis=2)) + own_factor
        weights = lax.optimization_barrier(expo.astype(jnp.bfloat16)).astype(jnp.float32)
        numer = jnp.einsum('kgt,tkd->kgd', weights, value_heads.astype(jnp.float32))
        numer = numer + own_factor[:, :, None] * own_value[:, None, :]
        result = (numer / total[:, :, None]).reshape(HEADS * HEAD).astype(jnp.bfloat16)
        return (cache, result)
    kv_cache, read_out = lax.map(one_prompt, (tokens, cum_gate, new_gate, new_query, new_kv))
    return (kv_cache, cum_gate, read_out)
```

```python
import functools
import math

import jax
import jax.numpy as jnp
from jax import lax
from jax.experimental import pallas as pl
from jax.experimental.pallas import tpu as pltpu
from jax.sharding import PartitionSpec as P

HEAD = 64
CORES = 2
MESH = pl.DeviceIdType.MESH


def row_parts(rows):
    first = max(16, (rows * 13 // 16) // 16 * 16)
    return [(0, first), (first, rows - first)] if first < rows else [(0, rows)]


def kernel(
    sp_size, tp_size, x_size, chunks,
    tok_hbm, gain_ref, wk_hbm, wv_hbm, gate_in, new_gate_ref, query_ref, new_kv_ref,
    kv_hbm, gate_out, read_ref,
    tok, wk, wv, both, scaled, acc, inv, proj, kv_buf, gates,
    in_sem, out_sem, tok_recv, tok_y_send, tok_c_send, w_recv, w_send, g_recv, g_send,
):
    z_size, y_size = sp_size // x_size, tp_size // CORES
    rows, width = wk_hbm.shape
    positions, depth = tok_hbm.shape[1:]
    part = positions // chunks
    parts = row_parts(rows)
    kinds = 2 * len(parts)
    sp, tp = lax.axis_index("sp"), lax.axis_index("tp")
    z, x = sp // x_size, lax.rem(sp, x_size)
    y, core = tp // CORES, lax.rem(tp, CORES)
    other_core = y * CORES + (CORES - 1 - core)

    loads = [
        pltpu.make_async_copy(wk_hbm, wk.at[sp], in_sem.at[0]),
        pltpu.make_async_copy(wv_hbm, wv.at[sp], in_sem.at[1]),
        pltpu.make_async_copy(tok_hbm.at[0], tok.at[tp], in_sem.at[2]),
        pltpu.make_async_copy(gate_in.at[tp], gates.at[tp], in_sem.at[3]),
    ]
    for load in loads:
        load.start()

    x_peers = [lax.rem(x + i, x_size) for i in range(1, x_size)]
    tp_peers = [lax.rem(tp + i, tp_size) for i in range(1, tp_size)]
    above, below = z + 1 < z_size, z >= 1

    barrier = pltpu.get_barrier_semaphore()

    def greet(device):
        pl.semaphore_signal(barrier, inc=1, device_id=device, device_id_type=MESH)

    for peer in tp_peers:
        greet({"sp": sp, "tp": peer})
    for peer in x_peers:
        greet({"sp": z * x_size + peer, "tp": tp})
    pl.when(above)(lambda: greet({"sp": sp + x_size, "tp": tp}))
    pl.when(below)(lambda: greet({"sp": sp - x_size, "tp": tp}))
    pl.semaphore_wait(
        barrier,
        tp_size - 1 + x_size - 1 + above.astype(jnp.int32) + below.astype(jnp.int32),
    )

    sends = []

    def start(copy, cond=None):
        sends.append((copy, cond))
        if cond is None:
            copy.start()
        else:
            pl.when(cond)(copy.start)

    def weight(kind, block):
        first, size = parts[kind // 2]
        return (wk, wv)[kind % 2].at[block, pl.ds(first, size), :]

    def weight_copy(kind, block, way, device_sp):
        return pltpu.make_async_remote_copy(
            src_ref=weight(kind, block),
            dst_ref=weight(kind, block),
            send_sem=w_send.at[kind, block, way],
            recv_sem=w_recv.at[kind, block],
            device_id={"sp": device_sp, "tp": tp},
            device_id_type=MESH,
        )

    def send_up(kind, block, cond):
        start(weight_copy(kind, block, 0, sp + x_size), cond)

    def send_down(kind, block, cond):
        start(weight_copy(kind, block, 1, sp - x_size), cond)

    def send_x(kind, block, cond=None):
        for i, peer in enumerate(x_peers):
            start(weight_copy(kind, block, 2 + i, z * x_size + peer), cond)

    def wait_weight(kind, block, cond=None):
        copy = weight_copy(kind, block, 0, sp)
        if cond is None:
            copy.wait_recv()
        else:
            pl.when(cond)(copy.wait_recv)

    def tok_copy(owner, chunk, send_sem, device_tp):
        piece = tok.at[owner, pl.ds(chunk * part, part), :]
        return pltpu.make_async_remote_copy(
            src_ref=piece,
            dst_ref=piece,
            send_sem=send_sem,
            recv_sem=tok_recv.at[owner, chunk],
            device_id={"sp": sp, "tp": device_tp},
            device_id_type=MESH,
        )

    y_peers = [lax.rem(y + i, y_size) for i in range(1, y_size)]

    loads[0].wait()
    loads[1].wait()
    late_kinds = list(range(2, kinds))
    for kind in late_kinds + [0, 1]:
        send_x(kind, sp)
    for kind in range(kinds):
        send_up(kind, sp, above)
        send_down(kind, sp, below)
    loads[2].wait()
    for chunk in range(chunks):
        for i, peer in enumerate(y_peers):
            start(tok_copy(tp, chunk, tok_y_send.at[i, chunk], peer * CORES + core))
        start(tok_copy(tp, chunk, tok_c_send.at[0, chunk], other_core))
    for i, peer in enumerate(tp_peers):
        start(
            pltpu.make_async_remote_copy(
                src_ref=gate_in.at[peer],
                dst_ref=gates.at[tp],
                send_sem=g_send.at[i],
                recv_sem=g_recv.at[tp],
                device_id={"sp": sp, "tp": peer},
                device_id_type=MESH,
            )
        )

    def scale_rows(owner, first, size):
        piece = tok[owner, pl.ds(first, size), :].astype(jnp.float32)
        square = jnp.mean(piece * piece, axis=-1, keepdims=True)
        inv[owner, pl.ds(first, size), :] = lax.rsqrt(square + 1e-06)
        out = (piece * gain_ref[...]).astype(jnp.bfloat16)
        for s in range(sp_size):
            scaled[s, owner, pl.ds(first, size), :] = out[:, s * rows:(s + 1) * rows]

    def scale_chunk(owner, chunk):
        @pl.loop(0, part // 16)
        def _(i):
            scale_rows(owner, chunk * part + i * 16, 16)

    def pair(block):
        keys, values = wk[block], wv[block]
        pieces = []
        for k in range(width // HEAD):
            pieces += [keys[:, k * HEAD:(k + 1) * HEAD], values[:, k * HEAD:(k + 1) * HEAD]]
        both[block] = jnp.concatenate(pieces, axis=1)

    def add(block, owner):
        acc[owner] += jnp.dot(
            scaled[block, owner], both[block], preferred_element_type=jnp.float32
        )

    def add_near(block):
        pair(block)
        add(block, tp)
        add(block, other_core)

    @pl.loop(0, tp_size)
    def _(i):
        acc[i] = jnp.zeros(acc.shape[1:], jnp.float32)

    for chunk in range(chunks):
        scale_chunk(tp, chunk)
    for chunk in range(chunks):
        tok_copy(other_core, chunk, tok_c_send.at[0, chunk], other_core).wait_recv()
        scale_chunk(other_core, chunk)
    add_near(sp)

    far_owners = [(peer * CORES + core, peer * CORES + (CORES - 1 - core)) for peer in y_peers]

    def pass_tokens(chunk):
        for i, (same, _) in enumerate(far_owners):
            tok_copy(same, chunk, tok_c_send.at[0, chunk], other_core).wait_recv()
            start(tok_copy(same, chunk, tok_c_send.at[1 + i, chunk], other_core))

    def scale_far(chunk):
        for same, cross in far_owners:
            scale_chunk(same, chunk)
            tok_copy(cross, chunk, tok_c_send.at[0, chunk], other_core).wait_recv()
            scale_chunk(cross, chunk)

    reach = jnp.maximum(z, z_size - 1 - z)

    def take_z(d):
        low, high = z - d >= 0, z + d < z_size
        below_block, above_block = sp - d * x_size, sp + d * x_size
        for kind in range(kinds):
            if kind < 2:
                wait_weight(kind, below_block, low)
                send_up(kind, below_block, low & above)
                send_x(kind, below_block, low)
                wait_weight(kind, above_block, high)
                send_down(kind, above_block, high & below)
                send_x(kind, above_block, high)
            else:
                for column in [x] + x_peers:
                    low_block = (z - d) * x_size + column
                    high_block = (z + d) * x_size + column
                    wait_weight(kind, low_block, low)
                    send_up(kind, low_block, low & above)
                    wait_weight(kind, high_block, high)
                    send_down(kind, high_block, high & below)

        @pl.when(low)
        def _():
            add_near(below_block)

        @pl.when(high)
        def _():
            add_near(above_block)

    def take_x(d, now, use):
        for sign in (-1, 1):
            there = (z + sign * d >= 0) & (z + sign * d < z_size) & now
            for column in x_peers:
                block = (z + sign * d) * x_size + column

                @pl.when(there)
                def _(block=block):
                    for kind in range(2):
                        wait_weight(kind, block)
                    use(block)

    steps = max(z_size - 1, 1)
    passed = 0
    for d in range(1, z_size):
        if d == 1:
            for column in x_peers:
                for kind in late_kinds:
                    block = z * x_size + column
                    wait_weight(kind, block)
                    send_up(kind, block, above)
                    send_down(kind, block, below)
            while passed < 1:
                pass_tokens(passed)
                passed += 1
        take_z(d)
        if d == 1:
            for column in x_peers:
                block = z * x_size + column
                for kind in range(2):
                    wait_weight(kind, block)
                add_near(block)
        else:
            take_x(d - 1, d - 1 < reach, add_near)
        while passed < min(chunks - 1, 1 + d * (chunks - 1) // steps):
            pass_tokens(passed)
            passed += 1
    while passed < chunks:
        pass_tokens(passed)
        passed += 1
    for chunk in range(chunks):
        scale_far(chunk)

    @pl.loop(0, sp_size)
    def _(block):
        far = (jnp.abs(block // x_size - z) == reach) & (lax.rem(block, x_size) != x)

        @pl.when(jnp.logical_not(far))
        def _():
            for owners in far_owners:
                for owner in owners:
                    add(block, owner)

    def add_all(block):
        pair(block)

        @pl.loop(0, tp_size)
        def _(owner):
            add(block, owner)

    loads[3].wait()
    for peer in tp_peers:
        pltpu.make_async_remote_copy(
            src_ref=gate_in.at[peer],
            dst_ref=gates.at[peer],
            send_sem=g_send.at[0],
            recv_sem=g_recv.at[peer],
            device_id={"sp": sp, "tp": peer},
            device_id_type=MESH,
        ).wait_recv()
    heads = gate_out.shape[1]
    kv_heads = width // HEAD
    group = heads // kv_heads
    lanes = max(heads, 8)
    gate = jnp.concatenate([gates[i] for i in range(tp_size)], axis=1)
    gate_out[0] = gate
    query = query_ref[...].astype(jnp.float32)
    fresh = new_kv_ref[0].astype(jnp.float32)
    fresh_gate = new_gate_ref[...]

    def padded(list_of_rows, fill):
        missing = lanes - heads
        if missing:
            list_of_rows = list_of_rows + [jnp.full((missing, fill), 0.0, jnp.float32)]
        return jnp.concatenate(list_of_rows, axis=0)

    query_rows = padded([query[:, h * HEAD:(h + 1) * HEAD] for h in range(heads)], HEAD)
    fresh_rows = padded([fresh[h // group:h // group + 1, :] for h in range(heads)], 2 * HEAD)
    scale_factor = 1.0 / math.sqrt(HEAD)
    own = jnp.sum(query_rows * fresh_rows[:, :HEAD], axis=1, keepdims=True) * scale_factor
    own_value = fresh_rows[:, HEAD:]
    pick = lax.broadcasted_iota(jnp.int32, (lanes, heads), 0) == lax.broadcasted_iota(
        jnp.int32, (lanes, heads), 1
    )
    gate_column = jnp.sum(jnp.where(pick, fresh_gate, 0.0), axis=1, keepdims=True)
    if lanes > heads:
        gate = jnp.concatenate(
            [gate, jnp.zeros((lanes - heads, gate.shape[1]), jnp.float32)], axis=0
        )
    bias = gate_column - gate
    head_of = lax.broadcasted_iota(jnp.int32, (lanes, 2 * HEAD), 0) // group
    wide = jnp.concatenate([query_rows, jnp.zeros_like(query_rows)], axis=1)
    wide = jnp.concatenate(
        [jnp.where(head_of == k, wide, 0.0) for k in range(kv_heads)], axis=1
    ).astype(jnp.bfloat16)

    for d in range(z_size):
        take_x(d, reach == d, add_all) if d else None

    for owner in range(tp_size):
        out = (acc[owner] * inv[owner]).astype(jnp.bfloat16)
        proj[pl.ds(owner * positions, positions), :] = out
        for k in range(kv_heads):
            kv_buf[0, k, pl.ds(owner * positions, positions), :] = out[
                :, 2 * k * HEAD:2 * (k + 1) * HEAD
            ]
    store = pltpu.make_async_copy(kv_buf, kv_hbm, out_sem)
    store.start()

    score = lax.dot_general(
        wide, proj[...], (((1,), (1,)), ((), ())), preferred_element_type=jnp.float32
    )
    score = score * scale_factor + bias
    top = jnp.maximum(jnp.max(score, axis=1, keepdims=True), own)
    expo = jnp.exp(score - top)
    own_factor = jnp.exp(own - top)
    total = jnp.sum(expo, axis=1, keepdims=True) + own_factor
    read = jnp.dot(expo.astype(jnp.bfloat16), proj[...], preferred_element_type=jnp.float32)
    value_of = lax.broadcasted_iota(jnp.int32, (lanes, HEAD), 0) // group
    numer = own_factor * own_value
    for k in range(kv_heads):
        numer += jnp.where(value_of == k, read[:, (2 * k + 1) * HEAD:(2 * k + 2) * HEAD], 0.0)
    result = numer / total
    read_ref[...] = jnp.concatenate(
        [result[h:h + 1, :] for h in range(heads)], axis=1
    ).astype(jnp.bfloat16)

    for copy, cond in sends:
        if cond is None:
            copy.wait_send()
        else:
            pl.when(cond)(copy.wait_send)
    store.wait()


def per_device(sp_size, tp_size, tokens, norm_gain, key_weight, value_weight, cum_gate, new_gate, new_query, new_kv):
    _, positions, depth = tokens.shape
    rows, width = key_weight.shape
    heads_all = cum_gate.shape[1]
    heads = heads_all // tp_size
    kv_heads = width // HEAD
    length = positions * tp_size
    x_size = 1 << (int(math.log2(sp_size)) // 2)
    chunks = 4
    kinds = 2 * len(row_parts(rows))
    y_size = tp_size // CORES
    any_spec = pl.BlockSpec(memory_space=pl.ANY)
    vmem = pl.BlockSpec(memory_space=pltpu.VMEM)
    dma = pltpu.SemaphoreType.DMA
    return pl.pallas_call(
        functools.partial(kernel, sp_size, tp_size, x_size, chunks),
        out_shape=(
            jax.ShapeDtypeStruct((1, kv_heads, length, 2 * HEAD), jnp.bfloat16),
            jax.ShapeDtypeStruct((1, heads, length), jnp.float32),
            jax.ShapeDtypeStruct((1, heads * HEAD), jnp.bfloat16),
        ),
        in_specs=[any_spec, vmem, any_spec, any_spec, vmem, vmem, vmem, vmem],
        out_specs=(any_spec, vmem, vmem),
        scratch_shapes=[
            pltpu.VMEM((tp_size, positions, depth), jnp.bfloat16),
            pltpu.VMEM((sp_size, rows, width), jnp.bfloat16),
            pltpu.VMEM((sp_size, rows, width), jnp.bfloat16),
            pltpu.VMEM((sp_size, rows, 2 * width), jnp.bfloat16),
            pltpu.VMEM((sp_size, tp_size, positions, rows), jnp.bfloat16),
            pltpu.VMEM((tp_size, positions, 2 * width), jnp.float32),
            pltpu.VMEM((tp_size, positions, 1), jnp.float32),
            pltpu.VMEM((length, 2 * width), jnp.bfloat16),
            pltpu.VMEM((1, kv_heads, length, 2 * HEAD), jnp.bfloat16),
            pltpu.VMEM((tp_size, heads, positions), jnp.float32),
            dma((4,)),
            dma,
            dma((tp_size, chunks)),
            dma((max(y_size - 1, 1), chunks)),
            dma((y_size, chunks)),
            dma((kinds, sp_size)),
            dma((kinds, sp_size, 1 + x_size)),
            dma((tp_size,)),
            dma((tp_size,)),
        ],
        compiler_params=pltpu.CompilerParams(
            collective_id=0, has_side_effects=True, vmem_limit_bytes=62 * 1024 * 1024
        ),
        name="prefill",
    )(
        tokens, norm_gain.reshape(1, depth), key_weight, value_weight,
        cum_gate.reshape(tp_size, heads, positions), new_gate, new_query, new_kv,
    )


def solution(mesh):
    in_specs = (
        P("sp", "tp", None),
        P(),
        P("sp", "tp"),
        P("sp", "tp"),
        P("sp", None, "tp"),
        P("sp", "tp"),
        P("sp", "tp"),
        P("sp", "tp", None),
    )
    out_specs = (P("sp", "tp", None, None), P("sp", "tp", None), P("sp", "tp"))
    return jax.shard_map(
        functools.partial(per_device, mesh.shape["sp"], mesh.shape["tp"]),
        mesh=mesh, in_specs=in_specs, out_specs=out_specs, check_vma=False,
    )
```

```python
import functools
import math

import jax
import jax.numpy as jnp
from jax import lax
from jax.experimental import pallas as pl
from jax.experimental.pallas import tpu as pltpu
from jax.sharding import PartitionSpec as P

HEAD = 64
CORES = 2
MESH = pl.DeviceIdType.MESH


def kernel(
    sp_size, tp_size, x_size, chunks,
    tok_hbm, gain_hbm, wk_hbm, wv_hbm, gate_hbm, new_gate_hbm, query_hbm, new_kv_hbm,
    kv_out, gate_out, bias_out, wide_out, own_out, own_value_out,
    gain_ref, gate_in, new_gate_ref, query_ref, new_kv_ref, tok, wk, wv, both, scaled, acc, inv, gates,
    in_sem, tok_recv, tok_y_send, tok_c_send, w_recv, w_send, g_recv, g_send,
):
    z_size, y_size = sp_size // x_size, tp_size // CORES
    rows, width = wk_hbm.shape
    positions, depth = tok_hbm.shape[1:]
    part = positions // chunks
    sp, tp = lax.axis_index("sp"), lax.axis_index("tp")
    z, x = sp // x_size, lax.rem(sp, x_size)
    y, core = tp // CORES, lax.rem(tp, CORES)
    other_core = y * CORES + (CORES - 1 - core)

    loads = [
        pltpu.make_async_copy(wk_hbm, wk.at[sp], in_sem.at[0]),
        pltpu.make_async_copy(wv_hbm, wv.at[sp], in_sem.at[1]),
        pltpu.make_async_copy(tok_hbm.at[0], tok.at[tp], in_sem.at[2]),
        pltpu.make_async_copy(gate_hbm, gate_in, in_sem.at[3]),
        pltpu.make_async_copy(gain_hbm, gain_ref, in_sem.at[4]),
        pltpu.make_async_copy(new_gate_hbm, new_gate_ref, in_sem.at[5]),
        pltpu.make_async_copy(query_hbm, query_ref, in_sem.at[6]),
        pltpu.make_async_copy(new_kv_hbm, new_kv_ref, in_sem.at[7]),
    ]
    for load in loads:
        load.start()

    x_peers = [lax.rem(x + i, x_size) for i in range(1, x_size)]
    tp_peers = [lax.rem(tp + i, tp_size) for i in range(1, tp_size)]
    above, below = z + 1 < z_size, z >= 1

    barrier = pltpu.get_barrier_semaphore()

    def greet(device):
        pl.semaphore_signal(barrier, inc=1, device_id=device, device_id_type=MESH)

    for peer in tp_peers:
        greet({"sp": sp, "tp": peer})
    for peer in x_peers:
        greet({"sp": z * x_size + peer, "tp": tp})
    pl.when(above)(lambda: greet({"sp": sp + x_size, "tp": tp}))
    pl.when(below)(lambda: greet({"sp": sp - x_size, "tp": tp}))
    pl.semaphore_wait(
        barrier,
        tp_size - 1 + x_size - 1 + above.astype(jnp.int32) + below.astype(jnp.int32),
    )

    sends = []

    def start(copy, cond=None):
        sends.append((copy, cond))
        if cond is None:
            copy.start()
        else:
            pl.when(cond)(copy.start)

    def weight(kind, block):
        return (wk, wv)[kind].at[block]

    def weight_copy(kind, block, way, device_sp):
        return pltpu.make_async_remote_copy(
            src_ref=weight(kind, block),
            dst_ref=weight(kind, block),
            send_sem=w_send.at[kind, block, way],
            recv_sem=w_recv.at[kind, block],
            device_id={"sp": device_sp, "tp": tp},
            device_id_type=MESH,
        )

    def send_up(kind, block, cond):
        start(weight_copy(kind, block, 0, sp + x_size), cond)

    def send_down(kind, block, cond):
        start(weight_copy(kind, block, 1, sp - x_size), cond)

    def send_x(kind, block, cond=None):
        for i, peer in enumerate(x_peers):
            start(weight_copy(kind, block, 2 + i, z * x_size + peer), cond)

    def wait_weight(kind, block, cond=None):
        copy = weight_copy(kind, block, 0, sp)
        if cond is None:
            copy.wait_recv()
        else:
            pl.when(cond)(copy.wait_recv)

    def tok_copy(owner, chunk, send_sem, device_tp):
        piece = tok.at[owner, pl.ds(chunk * part, part), :]
        return pltpu.make_async_remote_copy(
            src_ref=piece,
            dst_ref=piece,
            send_sem=send_sem,
            recv_sem=tok_recv.at[owner, chunk],
            device_id={"sp": sp, "tp": device_tp},
            device_id_type=MESH,
        )

    y_peers = [lax.rem(y + i, y_size) for i in range(1, y_size)]

    loads[0].wait()
    loads[1].wait()
    for kind in (1, 0):
        send_x(kind, sp)
    for kind in range(2):
        send_up(kind, sp, above)
        send_down(kind, sp, below)
    loads[2].wait()
    for chunk in range(chunks):
        for i, peer in enumerate(y_peers):
            start(tok_copy(tp, chunk, tok_y_send.at[i, chunk], peer * CORES + core))
        start(tok_copy(tp, chunk, tok_c_send.at[0, chunk], other_core))
    loads[3].wait()
    for i, peer in enumerate(tp_peers):
        start(
            pltpu.make_async_remote_copy(
                src_ref=gate_in.at[peer],
                dst_ref=gates.at[tp],
                send_sem=g_send.at[i],
                recv_sem=g_recv.at[tp],
                device_id={"sp": sp, "tp": peer},
                device_id_type=MESH,
            )
        )

    def scale_rows(owner, first, size):
        piece = tok[owner, pl.ds(first, size), :].astype(jnp.float32)
        square = jnp.mean(piece * piece, axis=-1, keepdims=True)
        inv[owner, pl.ds(first, size), :] = lax.rsqrt(square + 1e-06)
        out = (piece * gain_ref[...]).astype(jnp.bfloat16)
        for s in range(sp_size):
            scaled[s, owner, pl.ds(first, size), :] = out[:, s * rows:(s + 1) * rows]

    def scale_chunk(owner, chunk):
        @pl.loop(0, part // 16)
        def _(i):
            scale_rows(owner, chunk * part + i * 16, 16)

    def pair(block):
        keys, values = wk[block], wv[block]
        pieces = []
        for k in range(width // HEAD):
            pieces += [keys[:, k * HEAD:(k + 1) * HEAD], values[:, k * HEAD:(k + 1) * HEAD]]
        both[block] = jnp.concatenate(pieces, axis=1)

    def add(block, owner):
        acc[owner] += jnp.dot(
            scaled[block, owner], both[block], preferred_element_type=jnp.float32
        )

    def add_near(block):
        pair(block)
        add(block, tp)
        add(block, other_core)

    @pl.loop(0, tp_size)
    def _(i):
        acc[i] = jnp.zeros(acc.shape[1:], jnp.float32)

    loads[4].wait()
    for chunk in range(chunks):
        scale_chunk(tp, chunk)
    for chunk in range(chunks):
        tok_copy(other_core, chunk, tok_c_send.at[0, chunk], other_core).wait_recv()
        scale_chunk(other_core, chunk)
    add_near(sp)

    far_owners = [(peer * CORES + core, peer * CORES + (CORES - 1 - core)) for peer in y_peers]

    def pass_tokens(chunk):
        for i, (same, _) in enumerate(far_owners):
            tok_copy(same, chunk, tok_c_send.at[0, chunk], other_core).wait_recv()
            start(tok_copy(same, chunk, tok_c_send.at[1 + i, chunk], other_core))

    def scale_far(chunk):
        for same, cross in far_owners:
            scale_chunk(same, chunk)
            tok_copy(cross, chunk, tok_c_send.at[0, chunk], other_core).wait_recv()
            scale_chunk(cross, chunk)

    reach = jnp.maximum(z, z_size - 1 - z)

    def sides(d):
        return (sp - d * x_size, z - d >= 0), (sp + d * x_size, z + d < z_size)

    def ends(d):
        if z_size < 3:
            return False, False
        return z - d == 0, z + d == z_size - 1

    def no(flag):
        return True if flag is False else jnp.logical_not(flag)

    def take_first(d):
        (low_block, low), (high_block, high) = sides(d)
        low_end, high_end = ends(d)
        for kind in range(2):
            wait_weight(kind, low_block, low)
            send_up(kind, low_block, low & above)
            send_x(kind, low_block, low & no(low_end) if kind else low)
            wait_weight(kind, high_block, high)
            send_down(kind, high_block, high & below)
            send_x(kind, high_block, high & no(high_end) if kind else high)

    def take_late(d):
        if z_size < 3:
            return
        (low_block, _), (high_block, _) = sides(d)
        low_end, high_end = ends(d)
        for column in x_peers:
            wait_weight(1, low_block - x + column, low_end)
            send_up(1, low_block - x + column, low_end & above)
            wait_weight(1, high_block - x + column, high_end)
            send_down(1, high_block - x + column, high_end & below)

    def take_x(d, now, use):
        for (block, there), end in zip(sides(d), ends(d)):
            for column in x_peers:

                @pl.when(there & now)
                def _(block=block - x + column, end=end):
                    wait_weight(0, block)
                    if end is False:
                        wait_weight(1, block)
                    else:
                        pl.when(jnp.logical_not(end))(lambda: wait_weight(1, block))
                    use(block)

    passed = 0

    def pass_up_to(limit):
        nonlocal passed
        while passed < limit:
            pass_tokens(passed)
            if passed:
                scale_far(passed - 1)
            passed += 1

    for column in x_peers:
        block = z * x_size + column
        wait_weight(1, block)
        if z_size > 2:
            send_up(1, block, z == 0)
            send_down(1, block, z == z_size - 1)
    steps = max(z_size - 1, 1)
    for d in range(1, z_size):
        take_first(d)
        if d == 1:
            pass_up_to(1)
            for column in x_peers:
                wait_weight(0, z * x_size + column)
                add_near(z * x_size + column)
        for block, there in sides(d):

            @pl.when(there)
            def _(block=block):
                add_near(block)

        if d > 1:
            take_x(d - 1, d - 1 < reach, add_near)
        if d < z_size - 1:
            take_late(d)
        pass_up_to(min(chunks - 1, d * (chunks - 1) // steps))
    pass_up_to(chunks)
    scale_far(chunks - 1)

    @pl.loop(0, sp_size)
    def _(block):
        last = (jnp.abs(block // x_size - z) == reach) & (lax.rem(block, x_size) != x)

        @pl.when(jnp.logical_not(last))
        def _():
            for owners in far_owners:
                for owner in owners:
                    add(block, owner)

    def add_all(block):
        pair(block)

        @pl.loop(0, tp_size)
        def _(owner):
            add(block, owner)

    for peer in tp_peers:
        pltpu.make_async_remote_copy(
            src_ref=gate_in.at[peer],
            dst_ref=gates.at[peer],
            send_sem=g_send.at[0],
            recv_sem=g_recv.at[peer],
            device_id={"sp": sp, "tp": peer},
            device_id_type=MESH,
        ).wait_recv()
    kv_heads = width // HEAD
    gates[tp] = gate_in[tp]
    gate = jnp.concatenate([gates[i] for i in range(tp_size)], axis=1)
    gate_out[...] = gate
    for load in loads[5:]:
        load.wait()
    heads = gate_out.shape[0]
    group = heads // kv_heads
    lanes = max(heads, 8)
    query = query_ref[...].astype(jnp.float32)
    fresh = new_kv_ref[0].astype(jnp.float32)
    fresh_gate = new_gate_ref[...]

    def padded(list_of_rows, fill):
        missing = lanes - heads
        if missing:
            list_of_rows = list_of_rows + [jnp.full((missing, fill), 0.0, jnp.float32)]
        return jnp.concatenate(list_of_rows, axis=0)

    query_rows = padded([query[:, h * HEAD:(h + 1) * HEAD] for h in range(heads)], HEAD)
    fresh_rows = padded([fresh[h // group:h // group + 1, :] for h in range(heads)], 2 * HEAD)
    scale_factor = 1.0 / math.sqrt(HEAD)
    own = jnp.sum(query_rows * fresh_rows[:, :HEAD], axis=1, keepdims=True) * scale_factor
    own_value = fresh_rows[:, HEAD:]
    pick = lax.broadcasted_iota(jnp.int32, (lanes, heads), 0) == lax.broadcasted_iota(
        jnp.int32, (lanes, heads), 1
    )
    gate_column = jnp.sum(jnp.where(pick, fresh_gate, 0.0), axis=1, keepdims=True)
    if lanes > heads:
        gate = jnp.concatenate(
            [gate, jnp.zeros((lanes - heads, gate.shape[1]), jnp.float32)], axis=0
        )
    bias = gate_column - gate
    head_of = lax.broadcasted_iota(jnp.int32, (lanes, 2 * HEAD), 0) // group
    wide = jnp.concatenate([query_rows, jnp.zeros_like(query_rows)], axis=1)
    bias_out[...] = bias
    for k in range(kv_heads):
        wide_out[k] = jnp.where(head_of == k, wide, 0.0).astype(jnp.bfloat16)
    own_out[...] = jnp.broadcast_to(own, own_out.shape)
    own_value_out[...] = own_value

    if z_size > 1:
        take_late(z_size - 1)
    for d in range(1, z_size):
        take_x(d, reach == d, add_all)

    for owner in range(tp_size):
        out = (acc[owner] * inv[owner]).astype(jnp.bfloat16)
        for k in range(kv_heads):
            kv_out[k, pl.ds(owner * positions, positions), :] = out[
                :, 2 * k * HEAD:2 * (k + 1) * HEAD
            ]

    for copy, cond in sends:
        if cond is None:
            copy.wait_send()
        else:
            pl.when(cond)(copy.wait_send)


def read_kernel(kv, gate, bias_ref, wide, own_ref, own_value_ref, kv_hbm, gate_hbm, read_ref, sem):
    stores = [
        pltpu.make_async_copy(kv, kv_hbm.at[0], sem.at[0]),
        pltpu.make_async_copy(gate, gate_hbm.at[0], sem.at[1]),
    ]
    for store in stores:
        store.start()
    heads = gate.shape[0]
    kv_heads, lanes = wide.shape[:2]
    group = heads // kv_heads
    own, bias, own_value = own_ref[:, :1], bias_ref[...], own_value_ref[...]
    score = 0.0
    for k in range(kv_heads):
        score += lax.dot_general(
            wide[k], kv[k], (((1,), (1,)), ((), ())), preferred_element_type=jnp.float32
        )
    score = score * (1.0 / math.sqrt(HEAD)) + bias
    top = jnp.maximum(jnp.max(score, axis=1, keepdims=True), own)
    expo = jnp.exp(score - top)
    own_factor = jnp.exp(own - top)
    total = jnp.sum(expo, axis=1, keepdims=True) + own_factor
    weights = expo.astype(jnp.bfloat16)
    value_of = lax.broadcasted_iota(jnp.int32, (lanes, HEAD), 0) // group
    numer = own_factor * own_value
    for k in range(kv_heads):
        read = jnp.dot(weights, kv[k], preferred_element_type=jnp.float32)
        numer += jnp.where(value_of == k, read[:, HEAD:], 0.0)
    result = numer / total
    read_ref[...] = jnp.concatenate(
        [result[h:h + 1, :] for h in range(heads)], axis=1
    ).astype(jnp.bfloat16)
    for store in stores:
        store.wait()


def per_device(sp_size, tp_size, tokens, norm_gain, key_weight, value_weight, cum_gate, new_gate, new_query, new_kv):
    _, positions, depth = tokens.shape
    rows, width = key_weight.shape
    heads_all = cum_gate.shape[1]
    heads = heads_all // tp_size
    kv_heads = width // HEAD
    length = positions * tp_size
    x_size = 1 << (int(math.log2(sp_size)) // 2)
    chunks = 4
    y_size = tp_size // CORES
    any_spec = pl.BlockSpec(memory_space=pl.ANY)
    vmem = pl.BlockSpec(memory_space=pltpu.VMEM)
    dma = pltpu.SemaphoreType.DMA
    bf16, f32 = jnp.bfloat16, jnp.float32
    lanes = max(heads, 8)
    buffers = [
        ((1, depth), f32),
        ((tp_size, heads, positions), f32),
        ((1, heads), f32),
        ((1, heads * HEAD), bf16),
        ((1, kv_heads, 2 * HEAD), bf16),
        ((tp_size, positions, depth), bf16),
        ((sp_size, rows, width), bf16),
        ((sp_size, rows, width), bf16),
        ((sp_size, rows, 2 * width), bf16),
        ((sp_size, tp_size, positions, rows), bf16),
        ((tp_size, positions, 2 * width), f32),
        ((tp_size, positions, 1), f32),
        ((tp_size, heads, positions), f32),
    ]
    need = sum(
        math.prod(shape[:-1]) * -(-shape[-1] // 128) * 128 * jnp.dtype(kind).itemsize
        for shape, kind in buffers
    )
    results = pl.pallas_call(
        functools.partial(kernel, sp_size, tp_size, x_size, chunks),
        out_shape=(
            jax.ShapeDtypeStruct((kv_heads, length, 2 * HEAD), bf16),
            jax.ShapeDtypeStruct((heads, length), f32),
            jax.ShapeDtypeStruct((lanes, length), f32),
            jax.ShapeDtypeStruct((kv_heads, lanes, 2 * HEAD), bf16),
            jax.ShapeDtypeStruct((lanes, 2 * HEAD), f32),
            jax.ShapeDtypeStruct((lanes, HEAD), f32),
        ),
        in_specs=[pl.BlockSpec(memory_space=pltpu.HBM)] * 8,
        out_specs=(vmem,) * 6,
        scratch_shapes=[pltpu.VMEM(shape, kind) for shape, kind in buffers] + [
            dma((8,)),
            dma((tp_size, chunks)),
            dma((max(y_size - 1, 1), chunks)),
            dma((y_size, chunks)),
            dma((2, sp_size)),
            dma((2, sp_size, 1 + x_size)),
            dma((tp_size,)),
            dma((tp_size,)),
        ],
        compiler_params=pltpu.CompilerParams(
            collective_id=0, has_side_effects=True,
            vmem_limit_bytes=min(62 * 1024 * 1024, need + 6 * 1024 * 1024),
        ),
        name="prefill",
    )(
        *(
            pltpu.with_memory_space_constraint(array, pltpu.HBM)
            for array in (
                tokens, norm_gain.reshape(1, depth), key_weight, value_weight,
                cum_gate.reshape(tp_size, heads, positions), new_gate, new_query, new_kv,
            )
        )
    )
    return pl.pallas_call(
        read_kernel,
        out_shape=(
            jax.ShapeDtypeStruct((1, kv_heads, length, 2 * HEAD), bf16),
            jax.ShapeDtypeStruct((1, heads, length), f32),
            jax.ShapeDtypeStruct((1, heads * HEAD), bf16),
        ),
        in_specs=[vmem] * 6,
        out_specs=(any_spec, any_spec, vmem),
        scratch_shapes=[dma((2,))],
        compiler_params=pltpu.CompilerParams(vmem_limit_bytes=8 * 1024 * 1024),
        name="first_read",
    )(*results)


def solution(mesh):
    in_specs = (
        P("sp", "tp", None),
        P(),
        P("sp", "tp"),
        P("sp", "tp"),
        P("sp", None, "tp"),
        P("sp", "tp"),
        P("sp", "tp"),
        P("sp", "tp", None),
    )
    out_specs = (P("sp", "tp", None, None), P("sp", "tp", None), P("sp", "tp"))
    return jax.shard_map(
        functools.partial(per_device, mesh.shape["sp"], mesh.shape["tp"]),
        mesh=mesh, in_specs=in_specs, out_specs=out_specs, check_vma=False,
    )
```

```python
import functools
import math

import jax
import jax.numpy as jnp
from jax import lax
from jax.experimental import pallas as pl
from jax.experimental.pallas import tpu as pltpu
from jax.sharding import PartitionSpec as P

HEAD = 64
CORES = 2
MESH = pl.DeviceIdType.MESH


def kernel(
    sp_size, tp_size, x_size, chunks,
    tok_hbm, gain_hbm, wk_hbm, wv_hbm, gate_hbm, new_gate_hbm, query_hbm, new_kv_hbm,
    kv_out, gate_out, bias_out, wide_out, own_out, own_value_out,
    gain_ref, gate_in, new_gate_ref, query_ref, new_kv_ref, tok, wk, wv, both, scaled, acc, inv, gates,
    in_sem, tok_recv, tok_y_send, tok_c_send, w_recv, w_send, g_recv, g_send,
):
    z_size, y_size = sp_size // x_size, tp_size // CORES
    rows, width = wk_hbm.shape
    positions, depth = tok_hbm.shape[1:]
    part = positions // chunks
    sp, tp = lax.axis_index("sp"), lax.axis_index("tp")
    z, x = sp // x_size, lax.rem(sp, x_size)
    y, core = tp // CORES, lax.rem(tp, CORES)
    other_core = y * CORES + (CORES - 1 - core)

    loads = [
        pltpu.make_async_copy(wk_hbm, wk.at[sp], in_sem.at[0]),
        pltpu.make_async_copy(wv_hbm, wv.at[sp], in_sem.at[1]),
        pltpu.make_async_copy(tok_hbm.at[0], tok.at[tp], in_sem.at[2]),
        pltpu.make_async_copy(gate_hbm, gate_in, in_sem.at[3]),
        pltpu.make_async_copy(gain_hbm, gain_ref, in_sem.at[4]),
        pltpu.make_async_copy(new_gate_hbm, new_gate_ref, in_sem.at[5]),
        pltpu.make_async_copy(query_hbm, query_ref, in_sem.at[6]),
        pltpu.make_async_copy(new_kv_hbm, new_kv_ref, in_sem.at[7]),
    ]
    for load in loads:
        load.start()

    x_peers = [lax.rem(x + i, x_size) for i in range(1, x_size)]
    tp_peers = [lax.rem(tp + i, tp_size) for i in range(1, tp_size)]
    above, below = z + 1 < z_size, z >= 1

    barrier = pltpu.get_barrier_semaphore()

    def greet(device):
        pl.semaphore_signal(barrier, inc=1, device_id=device, device_id_type=MESH)

    for peer in tp_peers:
        greet({"sp": sp, "tp": peer})
    for peer in x_peers:
        greet({"sp": z * x_size + peer, "tp": tp})
    pl.when(above)(lambda: greet({"sp": sp + x_size, "tp": tp}))
    pl.when(below)(lambda: greet({"sp": sp - x_size, "tp": tp}))
    pl.semaphore_wait(
        barrier,
        tp_size - 1 + x_size - 1 + above.astype(jnp.int32) + below.astype(jnp.int32),
    )

    sends = []

    def start(copy, cond=None):
        sends.append((copy, cond))
        if cond is None:
            copy.start()
        else:
            pl.when(cond)(copy.start)

    def weight(kind, block):
        return (wk, wv)[kind].at[block]

    def weight_copy(kind, block, way, device_sp):
        return pltpu.make_async_remote_copy(
            src_ref=weight(kind, block),
            dst_ref=weight(kind, block),
            send_sem=w_send.at[kind, block, way],
            recv_sem=w_recv.at[kind, block],
            device_id={"sp": device_sp, "tp": tp},
            device_id_type=MESH,
        )

    def send_up(kind, block, cond):
        start(weight_copy(kind, block, 0, sp + x_size), cond)

    def send_down(kind, block, cond):
        start(weight_copy(kind, block, 1, sp - x_size), cond)

    def send_x(kind, block, cond=None):
        for i, peer in enumerate(x_peers):
            start(weight_copy(kind, block, 2 + i, z * x_size + peer), cond)

    def wait_weight(kind, block, cond=None):
        copy = weight_copy(kind, block, 0, sp)
        if cond is None:
            copy.wait_recv()
        else:
            pl.when(cond)(copy.wait_recv)

    def tok_copy(owner, chunk, send_sem, device_tp):
        piece = tok.at[owner, pl.ds(chunk * part, part), :]
        return pltpu.make_async_remote_copy(
            src_ref=piece,
            dst_ref=piece,
            send_sem=send_sem,
            recv_sem=tok_recv.at[owner, chunk],
            device_id={"sp": sp, "tp": device_tp},
            device_id_type=MESH,
        )

    y_peers = [lax.rem(y + i, y_size) for i in range(1, y_size)]

    loads[0].wait()
    loads[1].wait()
    for kind in (1, 0):
        send_x(kind, sp)
    for kind in range(2):
        send_up(kind, sp, above)
        send_down(kind, sp, below)
    loads[2].wait()
    for chunk in range(chunks):
        for i, peer in enumerate(y_peers):
            start(tok_copy(tp, chunk, tok_y_send.at[i, chunk], peer * CORES + core))
        start(tok_copy(tp, chunk, tok_c_send.at[0, chunk], other_core))
    loads[3].wait()
    for i, peer in enumerate(tp_peers):
        start(
            pltpu.make_async_remote_copy(
                src_ref=gate_in.at[peer],
                dst_ref=gates.at[tp],
                send_sem=g_send.at[i],
                recv_sem=g_recv.at[tp],
                device_id={"sp": sp, "tp": peer},
                device_id_type=MESH,
            )
        )

    def scale_rows(owner, first, size):
        piece = tok[owner, pl.ds(first, size), :].astype(jnp.float32)
        square = jnp.mean(piece * piece, axis=-1, keepdims=True)
        inv[owner, pl.ds(first, size), :] = lax.rsqrt(square + 1e-06)
        out = (piece * gain_ref[...]).astype(jnp.bfloat16)
        for s in range(sp_size):
            scaled[s, owner, pl.ds(first, size), :] = out[:, s * rows:(s + 1) * rows]

    def scale_chunk(owner, chunk):
        @pl.loop(0, part // 16)
        def _(i):
            scale_rows(owner, chunk * part + i * 16, 16)

    def pair(block):
        keys, values = wk[block], wv[block]
        pieces = []
        for k in range(width // HEAD):
            pieces += [keys[:, k * HEAD:(k + 1) * HEAD], values[:, k * HEAD:(k + 1) * HEAD]]
        both[block] = jnp.concatenate(pieces, axis=1)

    def add(block, owner):
        acc[owner] += jnp.dot(
            scaled[block, owner], both[block], preferred_element_type=jnp.float32
        )

    def add_near(block):
        pair(block)
        add(block, tp)
        add(block, other_core)

    @pl.loop(0, tp_size)
    def _(i):
        acc[i] = jnp.zeros(acc.shape[1:], jnp.float32)

    loads[4].wait()
    for chunk in range(chunks):
        scale_chunk(tp, chunk)
    for chunk in range(chunks):
        tok_copy(other_core, chunk, tok_c_send.at[0, chunk], other_core).wait_recv()
        scale_chunk(other_core, chunk)
    add_near(sp)

    far_owners = [(peer * CORES + core, peer * CORES + (CORES - 1 - core)) for peer in y_peers]

    def pass_tokens(chunk):
        for i, (same, _) in enumerate(far_owners):
            tok_copy(same, chunk, tok_c_send.at[0, chunk], other_core).wait_recv()
            start(tok_copy(same, chunk, tok_c_send.at[1 + i, chunk], other_core))

    def scale_far(chunk):
        for same, cross in far_owners:
            scale_chunk(same, chunk)
            tok_copy(cross, chunk, tok_c_send.at[0, chunk], other_core).wait_recv()
            scale_chunk(cross, chunk)

    reach = jnp.maximum(z, z_size - 1 - z)

    def sides(d):
        return (sp - d * x_size, z - d >= 0), (sp + d * x_size, z + d < z_size)

    def ends(d):
        if z_size < 3:
            return False, False
        return z - d == 0, z + d == z_size - 1

    def no(flag):
        return True if flag is False else jnp.logical_not(flag)

    def take_first(d):
        (low_block, low), (high_block, high) = sides(d)
        low_end, high_end = ends(d)
        for kind in range(2):
            wait_weight(kind, low_block, low)
            send_up(kind, low_block, low & above)
            send_x(kind, low_block, low & no(low_end) if kind else low)
            wait_weight(kind, high_block, high)
            send_down(kind, high_block, high & below)
            send_x(kind, high_block, high & no(high_end) if kind else high)

    def take_late(d):
        if z_size < 3:
            return
        (low_block, _), (high_block, _) = sides(d)
        low_end, high_end = ends(d)
        for column in x_peers:
            wait_weight(1, low_block - x + column, low_end)
            send_up(1, low_block - x + column, low_end & above)
            wait_weight(1, high_block - x + column, high_end)
            send_down(1, high_block - x + column, high_end & below)

    def take_x(d, now, use):
        for (block, there), end in zip(sides(d), ends(d)):
            for column in x_peers:

                @pl.when(there & now)
                def _(block=block - x + column, end=end):
                    wait_weight(0, block)
                    if end is False:
                        wait_weight(1, block)
                    else:
                        pl.when(jnp.logical_not(end))(lambda: wait_weight(1, block))
                    use(block)

    passed = 0

    def pass_up_to(limit):
        nonlocal passed
        while passed < limit:
            pass_tokens(passed)
            if passed:
                scale_far(passed - 1)
            passed += 1

    for column in x_peers:
        block = z * x_size + column
        wait_weight(1, block)
        if z_size > 2:
            send_up(1, block, z == 0)
            send_down(1, block, z == z_size - 1)
    steps = max(z_size - 1, 1)
    for d in range(1, z_size):
        take_first(d)
        if d == 1:
            pass_up_to(1)
            for column in x_peers:
                wait_weight(0, z * x_size + column)
                add_near(z * x_size + column)
        for block, there in sides(d):

            @pl.when(there)
            def _(block=block):
                add_near(block)

        if d > 1:
            take_x(d - 1, d - 1 < reach, add_near)
        if d < z_size - 1:
            take_late(d)
        pass_up_to(min(chunks - 1, d * (chunks - 1) // steps))
    pass_up_to(chunks)
    scale_far(chunks - 1)

    @pl.loop(0, sp_size)
    def _(block):
        last = (jnp.abs(block // x_size - z) == reach) & (lax.rem(block, x_size) != x)

        @pl.when(jnp.logical_not(last))
        def _():
            for owners in far_owners:
                for owner in owners:
                    add(block, owner)

    def add_all(block):
        pair(block)

        @pl.loop(0, tp_size)
        def _(owner):
            add(block, owner)

    for peer in tp_peers:
        pltpu.make_async_remote_copy(
            src_ref=gate_in.at[peer],
            dst_ref=gates.at[peer],
            send_sem=g_send.at[0],
            recv_sem=g_recv.at[peer],
            device_id={"sp": sp, "tp": peer},
            device_id_type=MESH,
        ).wait_recv()
    kv_heads = width // HEAD
    gates[tp] = gate_in[tp]
    gate = jnp.concatenate([gates[i] for i in range(tp_size)], axis=1)
    gate_out[...] = gate
    for load in loads[5:]:
        load.wait()
    heads = gate_out.shape[0]
    group = heads // kv_heads
    lanes = max(heads, 8)
    query = query_ref[...].astype(jnp.float32)
    fresh = new_kv_ref[0].astype(jnp.float32)
    fresh_gate = new_gate_ref[...]

    def padded(list_of_rows, fill):
        missing = lanes - heads
        if missing:
            list_of_rows = list_of_rows + [jnp.full((missing, fill), 0.0, jnp.float32)]
        return jnp.concatenate(list_of_rows, axis=0)

    query_rows = padded([query[:, h * HEAD:(h + 1) * HEAD] for h in range(heads)], HEAD)
    fresh_rows = padded([fresh[h // group:h // group + 1, :] for h in range(heads)], 2 * HEAD)
    scale_factor = 1.0 / math.sqrt(HEAD)
    own = jnp.sum(query_rows * fresh_rows[:, :HEAD], axis=1, keepdims=True) * scale_factor
    own_value = fresh_rows[:, HEAD:]
    pick = lax.broadcasted_iota(jnp.int32, (lanes, heads), 0) == lax.broadcasted_iota(
        jnp.int32, (lanes, heads), 1
    )
    gate_column = jnp.sum(jnp.where(pick, fresh_gate, 0.0), axis=1, keepdims=True)
    if lanes > heads:
        gate = jnp.concatenate(
            [gate, jnp.zeros((lanes - heads, gate.shape[1]), jnp.float32)], axis=0
        )
    bias = gate_column - gate
    head_of = lax.broadcasted_iota(jnp.int32, (lanes, 2 * HEAD), 0) // group
    wide = jnp.concatenate([query_rows, jnp.zeros_like(query_rows)], axis=1)
    bias_out[...] = bias
    for k in range(kv_heads):
        wide_out[k] = jnp.where(head_of == k, wide, 0.0).astype(jnp.bfloat16)
    own_out[...] = jnp.broadcast_to(own, own_out.shape)
    own_value_out[...] = own_value

    if z_size > 1:
        take_late(z_size - 1)
    for d in range(1, z_size):
        take_x(d, reach == d, add_all)

    for owner in range(tp_size):
        out = (acc[owner] * inv[owner]).astype(jnp.bfloat16)
        for k in range(kv_heads):
            kv_out[k, pl.ds(owner * positions, positions), :] = out[
                :, 2 * k * HEAD:2 * (k + 1) * HEAD
            ]

    for copy, cond in sends:
        if cond is None:
            copy.wait_send()
        else:
            pl.when(cond)(copy.wait_send)


def read_kernel(kv, gate, bias_ref, wide, own_ref, own_value_ref, kv_hbm, gate_hbm, read_ref, sem):
    stores = [
        pltpu.make_async_copy(kv, kv_hbm.at[0], sem.at[0]),
        pltpu.make_async_copy(gate, gate_hbm.at[0], sem.at[1]),
    ]
    for store in stores:
        store.start()
    heads = gate.shape[0]
    kv_heads, lanes = wide.shape[:2]
    group = heads // kv_heads
    own, bias, own_value = own_ref[:, :1], bias_ref[...], own_value_ref[...]
    score = 0.0
    for k in range(kv_heads):
        score += lax.dot_general(
            wide[k], kv[k], (((1,), (1,)), ((), ())), preferred_element_type=jnp.float32
        )
    score = score * (1.0 / math.sqrt(HEAD)) + bias
    top = jnp.maximum(jnp.max(score, axis=1, keepdims=True), own)
    expo = jnp.exp(score - top)
    own_factor = jnp.exp(own - top)
    total = jnp.sum(expo, axis=1, keepdims=True) + own_factor
    weights = expo.astype(jnp.bfloat16)
    value_of = lax.broadcasted_iota(jnp.int32, (lanes, HEAD), 0) // group
    numer = own_factor * own_value
    for k in range(kv_heads):
        read = jnp.dot(weights, kv[k], preferred_element_type=jnp.float32)
        numer += jnp.where(value_of == k, read[:, HEAD:], 0.0)
    result = numer / total
    read_ref[...] = jnp.concatenate(
        [result[h:h + 1, :] for h in range(heads)], axis=1
    ).astype(jnp.bfloat16)
    for store in stores:
        store.wait()


def per_device(sp_size, tp_size, tokens, norm_gain, key_weight, value_weight, cum_gate, new_gate, new_query, new_kv):
    _, positions, depth = tokens.shape
    rows, width = key_weight.shape
    heads_all = cum_gate.shape[1]
    heads = heads_all // tp_size
    kv_heads = width // HEAD
    length = positions * tp_size
    x_size = 1 << (int(math.log2(sp_size)) // 2)
    chunks = 6
    y_size = tp_size // CORES
    any_spec = pl.BlockSpec(memory_space=pl.ANY)
    vmem = pl.BlockSpec(memory_space=pltpu.VMEM)
    dma = pltpu.SemaphoreType.DMA
    bf16, f32 = jnp.bfloat16, jnp.float32
    lanes = max(heads, 8)
    buffers = [
        ((1, depth), f32),
        ((tp_size, heads, positions), f32),
        ((1, heads), f32),
        ((1, heads * HEAD), bf16),
        ((1, kv_heads, 2 * HEAD), bf16),
        ((tp_size, positions, depth), bf16),
        ((sp_size, rows, width), bf16),
        ((sp_size, rows, width), bf16),
        ((sp_size, rows, 2 * width), bf16),
        ((sp_size, tp_size, positions, rows), bf16),
        ((tp_size, positions, 2 * width), f32),
        ((tp_size, positions, 1), f32),
        ((tp_size, heads, positions), f32),
    ]
    need = sum(
        math.prod(shape[:-1]) * -(-shape[-1] // 128) * 128 * jnp.dtype(kind).itemsize
        for shape, kind in buffers
    )
    results = pl.pallas_call(
        functools.partial(kernel, sp_size, tp_size, x_size, chunks),
        out_shape=(
            jax.ShapeDtypeStruct((kv_heads, length, 2 * HEAD), bf16),
            jax.ShapeDtypeStruct((heads, length), f32),
            jax.ShapeDtypeStruct((lanes, length), f32),
            jax.ShapeDtypeStruct((kv_heads, lanes, 2 * HEAD), bf16),
            jax.ShapeDtypeStruct((lanes, 2 * HEAD), f32),
            jax.ShapeDtypeStruct((lanes, HEAD), f32),
        ),
        in_specs=[pl.BlockSpec(memory_space=pltpu.HBM)] * 8,
        out_specs=(vmem,) * 6,
        scratch_shapes=[pltpu.VMEM(shape, kind) for shape, kind in buffers] + [
            dma((8,)),
            dma((tp_size, chunks)),
            dma((max(y_size - 1, 1), chunks)),
            dma((y_size, chunks)),
            dma((2, sp_size)),
            dma((2, sp_size, 1 + x_size)),
            dma((tp_size,)),
            dma((tp_size,)),
        ],
        compiler_params=pltpu.CompilerParams(
            collective_id=0, has_side_effects=True,
            vmem_limit_bytes=min(62 * 1024 * 1024, need + 6 * 1024 * 1024),
        ),
        name="prefill",
    )(
        *(
            pltpu.with_memory_space_constraint(array, pltpu.HBM)
            for array in (
                tokens, norm_gain.reshape(1, depth), key_weight, value_weight,
                cum_gate.reshape(tp_size, heads, positions), new_gate, new_query, new_kv,
            )
        )
    )
    return pl.pallas_call(
        read_kernel,
        out_shape=(
            jax.ShapeDtypeStruct((1, kv_heads, length, 2 * HEAD), bf16),
            jax.ShapeDtypeStruct((1, heads, length), f32),
            jax.ShapeDtypeStruct((1, heads * HEAD), bf16),
        ),
        in_specs=[vmem] * 6,
        out_specs=(any_spec, any_spec, vmem),
        scratch_shapes=[dma((2,))],
        compiler_params=pltpu.CompilerParams(vmem_limit_bytes=8 * 1024 * 1024),
        name="first_read",
    )(*results)


def solution(mesh):
    in_specs = (
        P("sp", "tp", None),
        P(),
        P("sp", "tp"),
        P("sp", "tp"),
        P("sp", None, "tp"),
        P("sp", "tp"),
        P("sp", "tp"),
        P("sp", "tp", None),
    )
    out_specs = (P("sp", "tp", None, None), P("sp", "tp", None), P("sp", "tp"))
    return jax.shard_map(
        functools.partial(per_device, mesh.shape["sp"], mesh.shape["tp"]),
        mesh=mesh, in_specs=in_specs, out_specs=out_specs, check_vma=False,
    )
```
